32 devices in a mesh: fs: 8 (over z, x), tp: 4 (over y, core).
Axes of the slice: x: 2, y: 2, z: 4, core: 2. Of those that a mesh axis runs over, the one named last changes fastest.
Arguments:
- prompt_tokens: bfloat16 [6144, 2048], P('fs', 'tp'), may hold values from -6 to 6
- norm_gain: float32 [2048], P('fs'), may hold values from 0.1 to 1.9
- up_master: float32 [2048, 4096], P('fs', 'tp'), may hold values from -6 to 6
- down_master: float32 [2048, 4096], P('fs', 'tp'), may hold values from -6 to 6
Outputs:
- serve_up: bfloat16 [2048, 4096], P(None, 'tp')
- serve_down: bfloat16 [2048, 4096], P(None, 'tp')
- mixed: bfloat16 [6144, 2048], P('fs', 'tp')
The draws below stay inside these ranges and needn't reach their ends.
All inputs are finite; a program needn't handle non-finite values.
Results may differ from the reference program's by a relative error of at most 0.009.
Values may be sent and summed in bfloat16 or wider, within the bound.
A program may use at most 64 MiB of HBM per device.

```python
import jax
import jax.numpy as jnp
from jax import lax

D = 2048
FF = 4096
TOK_DEV = 768
TOKENS = 6144
N_FS = 8
N_TP = 4


def steps_of(own_key, extent, shards, low, high):
    level = 1.0
    for dim, shards_of in shards:
        heights = jax.random.uniform(jax.random.fold_in(jax.random.fold_in(own_key, 6), dim), (shards_of,), jnp.float32, low / len(shards), high / len(shards))
        level = level * jnp.repeat(jnp.exp(heights), extent[dim] // shards_of).reshape((-1,) + (1,) * (len(extent) - 1 - dim))
    return level


def centred(own_key, shape, deviation, most, split=(), held_as=jnp.bfloat16):
    values = jax.random.normal(own_key, shape, jnp.float32) * deviation
    if len(split) > 0:
        values = steps_of(own_key, shape, split, -0.22, 0.18) * values
    return jnp.clip(values, min=-most, max=most).astype(held_as)


def setup_inputs(seed: int = 0) -> dict:
    arg_keys = jax.random.split(jax.random.key(seed), 5)
    prompt_tokens = centred(arg_keys[0], (TOKENS, D), 1.0, 6.0, ((0, 8), (1, 4)))
    norm_gain = jnp.clip(1.0 + 0.18 * jax.random.normal(arg_keys[1], (D,), jnp.float32), 0.1, 1.9)
    up_master = centred(arg_keys[2], (D, FF), 1.0, 6.0, ((0, 8), (1, 4)), jnp.float32)
    down_master = centred(arg_keys[3], (D, FF), 1.0, 6.0, ((0, 8), (1, 4)), jnp.float32)
    return dict(prompt_tokens=prompt_tokens, norm_gain=norm_gain, up_master=up_master, down_master=down_master)


def reference(prompt_tokens, norm_gain, up_master, down_master):
    serve_up = (norm_gain[:, None] * up_master).astype(jnp.bfloat16)
    serve_down = down_master.astype(jnp.bfloat16)
    group = FF // N_TP
    blocks = prompt_tokens.reshape(N_FS, TOK_DEV, D)

    def one_block(block):
        wide = block.astype(jnp.float32)
        normed = (wide * lax.rsqrt(lax.optimization_barrier(jnp.mean(wide * wide, axis=1, keepdims=True)) + 1e-05)).astype(jnp.bfloat16)
        hidden = jnp.dot(normed, serve_up, preferred_element_type=jnp.float32) * D ** (-0.5)
        act = jnp.square(jax.nn.relu(hidden)).astype(jnp.bfloat16)
        total = jnp.zeros((TOK_DEV, D), jnp.float32)
        for index in range(N_TP):
            act_part = act[:, index * group:(index + 1) * group]
            down_part = serve_down[:, index * group:(index + 1) * group]
            partial_value = lax.dot_general(act_part, down_part, (((1,), (1,)), ((), ())), preferred_element_type=jnp.float32) * FF ** (-0.5)
            total = total + partial_value.astype(jnp.bfloat16).astype(jnp.float32)
        return total.astype(jnp.bfloat16)
    mixed = lax.map(one_block, blocks).reshape(TOKENS, D)
    return (serve_up, serve_down, mixed)
```

```python
import functools

import jax
import jax.numpy as jnp
from jax import lax
from jax.experimental import pallas as pl
from jax.experimental.pallas import tpu as pltpu
from jax.sharding import PartitionSpec as P

MESH = pl.DeviceIdType.MESH
LANES = 128


def plain(prompt_tokens, norm_gain, up_master, down_master):
    up_folded = (norm_gain[:, None] * up_master).astype(jnp.bfloat16)
    down_cast = down_master.astype(jnp.bfloat16)
    whole = lax.all_gather(prompt_tokens, "tp", axis=1, tiled=True)
    width = whole.shape[1]
    hidden_units = up_master.shape[1] * lax.axis_size("tp")
    wide = whole.astype(jnp.float32)
    normed = (wide * lax.rsqrt(jnp.mean(wide * wide, axis=1, keepdims=True) + 1e-05)).astype(
        jnp.bfloat16
    )
    contract = (((1,), (1,)), ((), ()))
    serve_up, serve_down = (
        lax.all_gather(up_folded, "fs", axis=0, tiled=True),
        lax.all_gather(down_cast, "fs", axis=0, tiled=True),
    )
    hidden = jnp.dot(normed, serve_up, preferred_element_type=jnp.float32)
    act = jnp.square(jax.nn.relu(hidden * width ** (-0.5))).astype(jnp.bfloat16)
    product = lax.dot_general(act, serve_down, contract, preferred_element_type=jnp.float32)
    partial_value = (product * hidden_units ** (-0.5)).astype(jnp.bfloat16)
    mixed = lax.psum_scatter(partial_value, "tp", scatter_dimension=1, tiled=True)
    return (serve_up, serve_down, mixed)


def kernel(line, pieces, tok, gain, up, down, out_up, out_down, mixed,
           wu, wd, xt, xn, act, part, pbuf, psum, rin_p, rin_y,
           w_send, w_recv, t_send, t_recv, a_send, a_recv, b_send, b_recv, c_send, c_recv,
           o_sem, l_sem):
    T, dl = tok.shape
    r, F = up.shape
    D = wu.shape[0]
    tp = lax.axis_index("tp")
    fs = lax.axis_index("fs")
    z, x = fs // 2, fs % 2
    core, chip = tp % 2, tp // 2
    partner = tp + 1 - 2 * core
    mirror = (tp + 2) % 4
    diag = (partner + 2) % 4
    has_up, has_dn = z < line - 1, z > 0
    W = (wu, wd)
    nb = dl // LANES
    per = r // LANES
    half = T // 2
    zdev = ((fs + 2, tp), (fs - 2, tp), (fs + 1 - 2 * x, tp))

    barrier = pltpu.get_barrier_semaphore()

    def greet(dev):
        pl.semaphore_signal(barrier, inc=1, device_id=dev, device_id_type=MESH)

    for other in (partner, mirror, diag):
        greet((fs, other))
    greet(zdev[2])
    pl.when(has_up)(lambda: greet(zdev[0]))
    pl.when(has_dn)(lambda: greet(zdev[1]))

    base = pl.multiple_of(fs * r, r)
    for i in range(r // LANES):
        rows = slice(i * LANES, (i + 1) * LANES)
        g = jnp.transpose(jnp.broadcast_to(gain[:, rows], (LANES, LANES)))
        for c in range(F // LANES):
            cols = slice(c * LANES, (c + 1) * LANES)
            wu[pl.ds(base + i * LANES, LANES), cols] = (g * up[rows, cols]).astype(jnp.bfloat16)
    wd[pl.ds(base, r), :] = down[...].astype(jnp.bfloat16)
    own_tok = pltpu.make_async_copy(tok, xt.at[tp], l_sem)
    own_tok.start()
    links = 4 + has_up.astype(jnp.int32) + has_dn.astype(jnp.int32)
    pl.semaphore_wait(barrier, links)

    def piece(a, s, p, way):
        start, size = pieces[p][0], pieces[p][1]
        ref = W[a].at[pl.ds(pl.multiple_of(s * r + start, 16), size), :]
        return pltpu.make_async_remote_copy(
            src_ref=ref, dst_ref=ref, send_sem=w_send.at[way, a, s, p],
            recv_sem=w_recv.at[a, s, p], device_id=zdev[way], device_id_type=MESH)

    def tok_copy(src, k, slot, to):
        return pltpu.make_async_remote_copy(
            src_ref=src, dst_ref=xt.at[k], send_sem=t_send.at[slot], recv_sem=t_recv.at[k],
            device_id=(fs, to), device_id_type=MESH)

    one = [p for p in range(len(pieces)) if pieces[p][2] == 1]
    two = [p for p in range(len(pieces)) if pieces[p][2] == 2]

    def start(d):
        d.start()

    def wait_send(d):
        d.wait_send()

    def own_z(a, do):
        for p in one + two:
            pl.when(has_up)(lambda: do(piece(a, fs, p, 0)))
            pl.when(has_dn)(lambda: do(piece(a, fs, p, 1)))

    def own_x(a, do):
        for p in two + one:
            do(piece(a, fs, p, 2))

    xs = fs + 1 - 2 * x

    def cross(a, do, wait):
        for p in two:
            if wait:
                piece(a, xs, p, 2).wait_recv()
            pl.when(has_up)(lambda: do(piece(a, xs, p, 0)))
            pl.when(has_dn)(lambda: do(piece(a, xs, p, 1)))

    def place(idx):
        got = jnp.int32(0)
        for i in range(line):
            order = sorted(range(line), key=lambda k: (abs(k - i), k if i < line / 2 else -k))
            for q in range(line):
                got = got + jnp.where((z == i) & (idx == q), jnp.int32(order[q]), jnp.int32(0))
        return got

    def relay(a, idx, do, wait):
        zz = place(idx)
        onward_up = (zz < z) & has_up
        onward_dn = (zz > z) & has_dn
        same, cross_s = zz * 2 + x, zz * 2 + 1 - x
        for p in one:
            if wait:
                piece(a, same, p, 2).wait_recv()
            pl.when(onward_up)(lambda: do(piece(a, same, p, 0)))
            pl.when(onward_dn)(lambda: do(piece(a, same, p, 1)))
            do(piece(a, same, p, 2))
        for p in two:
            for s in (same, cross_s):
                if wait:
                    piece(a, s, p, 2).wait_recv()
                pl.when(onward_up)(lambda: do(piece(a, s, p, 0)))
                pl.when(onward_dn)(lambda: do(piece(a, s, p, 1)))

    tok_copy(tok, tp, 0, mirror).start()
    own_x(0, start)
    own_z(0, start)
    tok_copy(tok, tp, 1, partner).start()
    cross(0, start, True)
    for idx in range(1, line):
        relay(0, jnp.int32(idx), start, True)
        if idx == 1:
            tok_copy(tok, mirror, 0, mirror).wait_recv()
            tok_copy(xt.at[mirror], mirror, 2, partner).start()
    own_z(1, start)
    own_x(1, start)

    own_tok.wait()
    tok_copy(tok, partner, 1, partner).wait_recv()
    tok_copy(tok, diag, 1, partner).wait_recv()
    block = 64

    def norm(i, carry):
        rows = pl.ds(pl.multiple_of(i * block, block), block)
        wide = [xt[k, rows, :].astype(jnp.float32) for k in range(4)]
        sq = wide[0] * wide[0]
        for k in range(1, 4):
            sq = sq + wide[k] * wide[k]
        inv = lax.rsqrt(jnp.sum(sq, axis=1, keepdims=True) * (1.0 / D) + 1e-05)
        for k in range(4):
            xn[rows, k * dl:(k + 1) * dl] = (wide[k] * inv).astype(jnp.bfloat16)
        return carry

    lax.fori_loop(0, T // block, norm, 0)

    cross(1, start, True)
    for idx in range(line):
        s = place(jnp.int32(idx)) * 2 + 1 - x
        for p in one:
            piece(0, s, p, 2).wait_recv()
    up_out = pltpu.make_async_copy(wu, out_up, o_sem.at[line])
    up_out.start()

    mrows = LANES

    def first(i, carry):
        rows = pl.ds(pl.multiple_of(i * mrows, mrows), mrows)
        hidden = jnp.dot(xn[rows, :], wu[...], preferred_element_type=jnp.float32) * D ** (-0.5)
        hidden = jnp.maximum(hidden, 0.0)
        act[rows, :] = (hidden * hidden).astype(jnp.bfloat16)
        return carry

    lax.fori_loop(0, T // mrows, first, 0)
    relay(1, jnp.int32(1), start, True)

    scale = (F * 4) ** (-0.5)
    mine = pl.ds(pl.multiple_of(core * half, half), half)
    theirs = pl.ds(pl.multiple_of((1 - core) * half, half), half)
    steps = 2 * per

    def block_of(n):
        zz, j = place(n // steps), n % steps
        side = j // per
        s = zz * 2 + x + side * (1 - 2 * x)
        return s * per + j % per

    def owner_of(b):
        o = b // nb
        return o, (o // 2) == chip

    def to_partner(b):
        return pltpu.make_async_remote_copy(
            src_ref=part.at[b], dst_ref=rin_p.at[b % nb], send_sem=a_send.at[b],
            recv_sem=a_recv.at[b % nb], device_id=(fs, partner), device_id_type=MESH)

    def swap(b):
        return pltpu.make_async_remote_copy(
            src_ref=part.at[b, theirs, :], dst_ref=pbuf.at[b], send_sem=b_send.at[b],
            recv_sem=b_recv.at[b], device_id=(fs, partner), device_id_type=MESH)

    def to_owner(b, o):
        return pltpu.make_async_remote_copy(
            src_ref=psum.at[b], dst_ref=rin_y.at[b % nb, mine, :], send_sem=c_send.at[b],
            recv_sem=c_recv.at[b % nb, core], device_id=(fs, o), device_id_type=MESH)

    def second_half(b):
        o, here = owner_of(b)

        @pl.when(jnp.logical_not(here))
        def _():
            swap(b).wait_recv()
            psum[b] = (part[b, mine, :].astype(jnp.float32)
                       + pbuf[b].astype(jnp.float32)).astype(jnp.bfloat16)
            to_owner(b, o).start()

    def out_copy(idx):
        rows = pl.ds(pl.multiple_of(place(idx) * 2 * r, 2 * r), 2 * r)
        return pltpu.make_async_copy(wd.at[rows, :], out_down.at[rows, :], o_sem.at[idx])

    def body(n, carry):
        idx, j = n // steps, n % steps

        @pl.when((j == 0) & (idx >= 1) & (idx + 1 < line))
        def _():
            relay(1, idx + 1, start, True)

        far = place(idx) * 2 + 1 - x
        for h in range(per):
            @pl.when(j == per + h)
            def _():
                for p in one:
                    if pieces[p][0] // LANES == h:
                        piece(1, far, p, 2).wait_recv()
        b = block_of(n)
        rhs = wd[pl.ds(pl.multiple_of(b * LANES, LANES), LANES), :]
        product = lax.dot_general(act[...], rhs, (((1,), (1,)), ((), ())),
                                  preferred_element_type=jnp.float32)
        part[b] = (product * scale).astype(jnp.bfloat16)
        o, here = owner_of(b)

        @pl.when(here & (o != tp))
        def _():
            to_partner(b).start()

        @pl.when(jnp.logical_not(here))
        def _():
            swap(b).start()

        @pl.when(j == steps - 1)
        def _():
            out_copy(idx).start()

        @pl.when(n > 0)
        def _():
            second_half(block_of(n - 1))

        return carry

    total = line * steps
    lax.fori_loop(0, total, body, 0)
    second_half(block_of(jnp.int32(total - 1)))

    for i in range(nb):
        b = tp * nb + i
        to_partner(b).wait_recv()
        for c in range(2):
            pltpu.make_async_remote_copy(
                src_ref=psum.at[b], dst_ref=rin_y.at[i, c * half:(c + 1) * half, :],
                send_sem=c_send.at[b], recv_sem=c_recv.at[i, c],
                device_id=(fs, partner), device_id_type=MESH).wait_recv()
        mixed[:, i * LANES:(i + 1) * LANES] = (
            part[b].astype(jnp.float32) + rin_p[i].astype(jnp.float32)
            + rin_y[i].astype(jnp.float32)).astype(jnp.bfloat16)

    for slot, (k, to) in enumerate(((tp, mirror), (tp, partner), (mirror, partner))):
        tok_copy(xt.at[k], k, slot, to).wait_send()
    for a in range(2):
        own_x(a, wait_send)
        own_z(a, wait_send)
        cross(a, wait_send, False)

    def drain(idx, carry):
        for a in range(2):
            relay(a, idx, wait_send, False)
        return carry

    lax.fori_loop(1, line, drain, 0)

    def drain_sums(b, carry):
        o, here = owner_of(b)

        @pl.when(here & (o != tp))
        def _():
            to_partner(b).wait_send()

        @pl.when(jnp.logical_not(here))
        def _():
            swap(b).wait_send()
            to_owner(b, o).wait_send()

        return carry

    lax.fori_loop(0, D // LANES, drain_sums, 0)
    up_out.wait()

    def drain_out(idx, carry):
        out_copy(idx).wait()
        return carry

    lax.fori_loop(0, line, drain_out, 0)


def cut(r):
    across = min(LANES - 16, max(16, (r * 3 // 16) // 16 * 16))
    got = []
    for first in range(0, r, LANES):
        rows = LANES if first + LANES < r else LANES - across
        if rows == LANES:
            got += [(first, LANES // 2, 1), (first + LANES // 2, LANES // 2, 1)]
        else:
            got += [(first, rows, 1)]
    return got + [(r - across, across, 2)]


def fused(n_fs, prompt_tokens, norm_gain, up_master, down_master):
    T, dl = prompt_tokens.shape
    r, F = up_master.shape
    D = r * n_fs
    line = n_fs // 2
    pieces = cut(r)
    nblk, nb, half = D // LANES, dl // LANES, T // 2
    bf = jnp.bfloat16
    dma = pltpu.SemaphoreType.DMA
    vmem = pl.BlockSpec(memory_space=pltpu.VMEM)
    hbm = pl.BlockSpec(memory_space=pl.ANY)
    return pl.pallas_call(
        functools.partial(kernel, line, pieces),
        out_shape=(jax.ShapeDtypeStruct((D, F), bf), jax.ShapeDtypeStruct((D, F), bf),
                   jax.ShapeDtypeStruct((T, dl), bf)),
        in_specs=[vmem] * 4,
        out_specs=(hbm, hbm, vmem),
        scratch_shapes=[
            pltpu.VMEM((D, F), bf), pltpu.VMEM((D, F), bf),
            pltpu.VMEM((4, T, dl), bf), pltpu.VMEM((T, D), bf), pltpu.VMEM((T, F), bf),
            pltpu.VMEM((nblk, T, LANES), bf), pltpu.VMEM((nblk, half, LANES), bf),
            pltpu.VMEM((nblk, half, LANES), bf),
            pltpu.VMEM((nb, T, LANES), bf), pltpu.VMEM((nb, T, LANES), bf),
            dma((3, 2, n_fs, len(pieces))), dma((2, n_fs, len(pieces))),
            dma((3,)), dma((4,)),
            dma((nblk,)), dma((nb,)), dma((nblk,)), dma((nblk,)), dma((nblk,)), dma((nb, 2)),
            dma((line + 1,)), dma,
        ],
        compiler_params=pltpu.CompilerParams(
            collective_id=0, has_side_effects=True, vmem_limit_bytes=56 * 2 ** 20),
    )(prompt_tokens, norm_gain.reshape(1, r), up_master, down_master)


def solution(mesh):
    n_fs, n_tp = mesh.shape["fs"], mesh.shape["tp"]

    def shards(prompt_tokens, norm_gain, up_master, down_master):
        T, dl = prompt_tokens.shape
        r = up_master.shape[0]
        fits = (n_tp == 4 and n_fs % 2 == 0 and n_fs >= 6 and r % LANES == 0
                and dl % LANES == 0 and T % (2 * LANES) == 0 and r * n_fs == dl * n_tp)
        if not fits:
            return plain(prompt_tokens, norm_gain, up_master, down_master)
        return fused(n_fs, prompt_tokens, norm_gain, up_master, down_master)

    return jax.shard_map(
        shards,
        mesh=mesh,
        in_specs=(P("fs", "tp"), P("fs"), P("fs", "tp"), P("fs", "tp")),
        out_specs=(P(None, "tp"), P(None, "tp"), P("fs", "tp")),
        check_vma=False,
    )
```

```python
import functools

import jax
import jax.numpy as jnp
from jax import lax
from jax.experimental import pallas as pl
from jax.experimental.pallas import tpu as pltpu
from jax.sharding import PartitionSpec as P

MESH = pl.DeviceIdType.MESH
LANES = 128


def plain(prompt_tokens, norm_gain, up_master, down_master):
    up_folded = (norm_gain[:, None] * up_master).astype(jnp.bfloat16)
    down_cast = down_master.astype(jnp.bfloat16)
    whole = lax.all_gather(prompt_tokens, "tp", axis=1, tiled=True)
    width = whole.shape[1]
    hidden_units = up_master.shape[1] * lax.axis_size("tp")
    wide = whole.astype(jnp.float32)
    normed = (wide * lax.rsqrt(jnp.mean(wide * wide, axis=1, keepdims=True) + 1e-05)).astype(
        jnp.bfloat16
    )
    contract = (((1,), (1,)), ((), ()))
    serve_up, serve_down = (
        lax.all_gather(up_folded, "fs", axis=0, tiled=True),
        lax.all_gather(down_cast, "fs", axis=0, tiled=True),
    )
    hidden = jnp.dot(normed, serve_up, preferred_element_type=jnp.float32)
    act = jnp.square(jax.nn.relu(hidden * width ** (-0.5))).astype(jnp.bfloat16)
    product = lax.dot_general(act, serve_down, contract, preferred_element_type=jnp.float32)
    partial_value = (product * hidden_units ** (-0.5)).astype(jnp.bfloat16)
    mixed = lax.psum_scatter(partial_value, "tp", scatter_dimension=1, tiled=True)
    return (serve_up, serve_down, mixed)


def kernel(line, pieces, tok, gain, up, down_hbm, wu, wd, mixed,
           xt, xn, act, part, pbuf, psum, rin_p, rin_y,
           w_send, w_recv, t_send, t_recv, a_send, a_recv, b_send, b_recv, c_send, c_recv,
           o_sem, l_sem, down, d_sem):
    T, dl = tok.shape
    r, F = up.shape
    D = wu.shape[0]
    tp = lax.axis_index("tp")
    fs = lax.axis_index("fs")
    z, x = fs // 2, fs % 2
    core, chip = tp % 2, tp // 2
    partner = tp + 1 - 2 * core
    mirror = (tp + 2) % 4
    diag = (partner + 2) % 4
    has_up, has_dn = z < line - 1, z > 0
    W = (wu, wd)
    nb = dl // LANES
    per = r // LANES
    half = T // 2
    zdev = ((fs + 2, tp), (fs - 2, tp), (fs + 1 - 2 * x, tp))

    own_tok = pltpu.make_async_copy(tok, xt.at[tp], l_sem)
    own_tok.start()
    own_down = pltpu.make_async_copy(down_hbm, down, d_sem)
    own_down.start()

    barrier = pltpu.get_barrier_semaphore()

    def greet(dev):
        pl.semaphore_signal(barrier, inc=1, device_id=dev, device_id_type=MESH)

    for other in (partner, mirror, diag):
        greet((fs, other))
    greet(zdev[2])
    pl.when(has_up)(lambda: greet(zdev[0]))
    pl.when(has_dn)(lambda: greet(zdev[1]))

    base = pl.multiple_of(fs * r, r)
    for i in range(r // LANES):
        rows = slice(i * LANES, (i + 1) * LANES)
        g = jnp.transpose(jnp.broadcast_to(gain[:, rows], (LANES, LANES)))
        for c in range(F // LANES):
            cols = slice(c * LANES, (c + 1) * LANES)
            wu[pl.ds(base + i * LANES, LANES), cols] = (g * up[rows, cols]).astype(jnp.bfloat16)
    links = 4 + has_up.astype(jnp.int32) + has_dn.astype(jnp.int32)
    pl.semaphore_wait(barrier, links)

    def piece(a, s, p, way):
        start, size = pieces[p][0], pieces[p][1]
        ref = W[a].at[pl.ds(pl.multiple_of(s * r + start, 16), size), :]
        return pltpu.make_async_remote_copy(
            src_ref=ref, dst_ref=ref, send_sem=w_send.at[way, a, s, p],
            recv_sem=w_recv.at[a, s, p], device_id=zdev[way], device_id_type=MESH)

    def tok_copy(src, k, slot, to):
        return pltpu.make_async_remote_copy(
            src_ref=src, dst_ref=xt.at[k], send_sem=t_send.at[slot], recv_sem=t_recv.at[k],
            device_id=(fs, to), device_id_type=MESH)

    one = [p for p in range(len(pieces)) if pieces[p][2] == 1]
    two = [p for p in range(len(pieces)) if pieces[p][2] == 2]

    def start(d):
        d.start()

    def wait_send(d):
        d.wait_send()

    def own_z(a, do):
        for p in one + two:
            pl.when(has_up)(lambda: do(piece(a, fs, p, 0)))
            pl.when(has_dn)(lambda: do(piece(a, fs, p, 1)))

    def own_x(a, do):
        for p in two + one:
            do(piece(a, fs, p, 2))

    xs = fs + 1 - 2 * x

    def cross(a, do, wait):
        for p in two:
            if wait:
                piece(a, xs, p, 2).wait_recv()
            pl.when(has_up)(lambda: do(piece(a, xs, p, 0)))
            pl.when(has_dn)(lambda: do(piece(a, xs, p, 1)))

    def place(idx):
        got = jnp.int32(0)
        for i in range(line):
            order = sorted(range(line), key=lambda k: (abs(k - i), -k if i < line / 2 else k))
            for q in range(line):
                got = got + jnp.where((z == i) & (idx == q), jnp.int32(order[q]), jnp.int32(0))
        return got

    def relay(a, idx, do, wait, early=True, late=True):
        zz = place(idx)
        onward_up = (zz < z) & has_up
        onward_dn = (zz > z) & has_dn
        same, cross_s = zz * 2 + x, zz * 2 + 1 - x
        for p in one:
            if not (early if pieces[p][0] < LANES else late):
                continue
            if wait:
                piece(a, same, p, 2).wait_recv()
            pl.when(onward_up)(lambda: do(piece(a, same, p, 0)))
            pl.when(onward_dn)(lambda: do(piece(a, same, p, 1)))
            do(piece(a, same, p, 2))
        for p in two if late else ():
            for s in (same, cross_s):
                if wait:
                    piece(a, s, p, 2).wait_recv()
                pl.when(onward_up)(lambda: do(piece(a, s, p, 0)))
                pl.when(onward_dn)(lambda: do(piece(a, s, p, 1)))

    own_x(0, start)
    own_z(0, start)
    own_tok.wait()
    tok_copy(xt.at[tp], tp, 0, mirror).start()
    tok_copy(xt.at[tp], tp, 1, partner).start()
    own_down.wait()
    wd[pl.ds(base, r), :] = down[...].astype(jnp.bfloat16)
    cross(0, start, True)
    for idx in range(1, line):
        relay(0, jnp.int32(idx), start, True)
        if idx == 1:
            tok_copy(xt.at[mirror], mirror, 0, mirror).wait_recv()
            tok_copy(xt.at[mirror], mirror, 2, partner).start()
    own_z(1, start)
    own_x(1, start)

    tok_copy(xt.at[partner], partner, 1, partner).wait_recv()
    tok_copy(xt.at[diag], diag, 1, partner).wait_recv()
    block = 64

    def norm(i, carry):
        rows = pl.ds(pl.multiple_of(i * block, block), block)
        wide = [xt[k, rows, :].astype(jnp.float32) for k in range(4)]
        sq = wide[0] * wide[0]
        for k in range(1, 4):
            sq = sq + wide[k] * wide[k]
        inv = lax.rsqrt(jnp.sum(sq, axis=1, keepdims=True) * (1.0 / D) + 1e-05)
        for k in range(4):
            xn[rows, k * dl:(k + 1) * dl] = (wide[k] * inv).astype(jnp.bfloat16)
        return carry

    lax.fori_loop(0, T // block, norm, 0)

    cross(1, start, True)
    for idx in range(line):
        s = place(jnp.int32(idx)) * 2 + 1 - x
        for p in one:
            piece(0, s, p, 2).wait_recv()

    mrows = 2 * LANES

    def first(i, carry):
        rows = pl.ds(pl.multiple_of(i * mrows, mrows), mrows)
        hidden = jnp.dot(xn[rows, :], wu[...], preferred_element_type=jnp.float32) * D ** (-0.5)
        hidden = jnp.maximum(hidden, 0.0)
        act[rows, :] = (hidden * hidden).astype(jnp.bfloat16)
        return carry

    lax.fori_loop(0, T // mrows, first, 0)

    scale = (F * 4) ** (-0.5)
    mine = pl.ds(pl.multiple_of(core * half, half), half)
    theirs = pl.ds(pl.multiple_of((1 - core) * half, half), half)
    steps = 2 * per

    def block_of(n):
        zz, j = place(n // steps), n % steps
        side = j // per
        s = zz * 2 + x + side * (1 - 2 * x)
        return s * per + j % per

    def owner_of(b):
        o = b // nb
        return o, (o // 2) == chip

    def to_partner(b):
        return pltpu.make_async_remote_copy(
            src_ref=part.at[b], dst_ref=rin_p.at[b % nb], send_sem=a_send.at[b],
            recv_sem=a_recv.at[b % nb], device_id=(fs, partner), device_id_type=MESH)

    def swap(b):
        return pltpu.make_async_remote_copy(
            src_ref=part.at[b, theirs, :], dst_ref=pbuf.at[b], send_sem=b_send.at[b],
            recv_sem=b_recv.at[b], device_id=(fs, partner), device_id_type=MESH)

    def to_owner(b, o):
        return pltpu.make_async_remote_copy(
            src_ref=psum.at[b], dst_ref=rin_y.at[b % nb, mine, :], send_sem=c_send.at[b],
            recv_sem=c_recv.at[b % nb, core], device_id=(fs, o), device_id_type=MESH)

    def second_half(b):
        o, here = owner_of(b)

        @pl.when(jnp.logical_not(here))
        def _():
            swap(b).wait_recv()
            psum[b] = (part[b, mine, :].astype(jnp.float32)
                       + pbuf[b].astype(jnp.float32)).astype(jnp.bfloat16)
            to_owner(b, o).start()

    def body(n, carry):
        idx, j = n // steps, n % steps

        @pl.when((j == per) & (idx + 1 < line))
        def _():
            relay(1, idx + 1, start, True, late=False)

        @pl.when((j == 1) & (idx >= 1))
        def _():
            relay(1, idx, start, True, early=False)

        far = place(idx) * 2 + 1 - x
        for h in range(per):
            @pl.when(j == per + h)
            def _():
                for p in one:
                    if pieces[p][0] // LANES == h:
                        piece(1, far, p, 2).wait_recv()
        b = block_of(n)
        rhs = wd[pl.ds(pl.multiple_of(b * LANES, LANES), LANES), :]
        product = lax.dot_general(act[...], rhs, (((1,), (1,)), ((), ())),
                                  preferred_element_type=jnp.float32)
        part[b] = (product * scale).astype(jnp.bfloat16)
        o, here = owner_of(b)

        @pl.when(here & (o != tp))
        def _():
            to_partner(b).start()

        @pl.when(jnp.logical_not(here))
        def _():
            swap(b).start()

        @pl.when(n > 0)
        def _():
            second_half(block_of(n - 1))

        return carry

    total = line * steps
    lax.fori_loop(0, total, body, 0)
    second_half(block_of(jnp.int32(total - 1)))

    for i in range(nb):
        b = tp * nb + i
        to_partner(b).wait_recv()
        for c in range(2):
            pltpu.make_async_remote_copy(
                src_ref=psum.at[b], dst_ref=rin_y.at[i, c * half:(c + 1) * half, :],
                send_sem=c_send.at[b], recv_sem=c_recv.at[i, c],
                device_id=(fs, partner), device_id_type=MESH).wait_recv()
        mixed[:, i * LANES:(i + 1) * LANES] = (
            part[b].astype(jnp.float32) + rin_p[i].astype(jnp.float32)
            + rin_y[i].astype(jnp.float32)).astype(jnp.bfloat16)

    for slot, (k, to) in enumerate(((tp, mirror), (tp, partner), (mirror, partner))):
        tok_copy(xt.at[k], k, slot, to).wait_send()
    for a in range(2):
        own_x(a, wait_send)
        own_z(a, wait_send)
        cross(a, wait_send, False)

    def drain(idx, carry):
        for a in range(2):
            relay(a, idx, wait_send, False)
        return carry

    lax.fori_loop(1, line, drain, 0)

    def drain_sums(b, carry):
        o, here = owner_of(b)

        @pl.when(here & (o != tp))
        def _():
            to_partner(b).wait_send()

        @pl.when(jnp.logical_not(here))
        def _():
            swap(b).wait_send()
            to_owner(b, o).wait_send()

        return carry

    lax.fori_loop(0, D // LANES, drain_sums, 0)


def cut(r):
    across = min(LANES - 16, max(16, (r * 3 // 16) // 16 * 16))
    got = []
    for first in range(0, r, LANES):
        rows = LANES if first + LANES < r else LANES - across
        if rows == LANES:
            got += [(first, LANES // 2, 1), (first + LANES // 2, LANES // 2, 1)]
        else:
            got += [(first, rows, 1)]
    return got + [(r - across, across, 2)]


def fused(n_fs, prompt_tokens, norm_gain, up_master, down_master):
    T, dl = prompt_tokens.shape
    r, F = up_master.shape
    D = r * n_fs
    line = n_fs // 2
    pieces = cut(r)
    nblk, nb, half = D // LANES, dl // LANES, T // 2
    bf = jnp.bfloat16
    dma = pltpu.SemaphoreType.DMA
    vmem = pl.BlockSpec(memory_space=pltpu.VMEM)
    hbm = pl.BlockSpec(memory_space=pl.ANY)
    return pl.pallas_call(
        functools.partial(kernel, line, pieces),
        out_shape=(pltpu.VMEM((D, F), bf), pltpu.VMEM((D, F), bf), pltpu.VMEM((T, dl), bf)),
        in_specs=[hbm, vmem, vmem, hbm],
        out_specs=(vmem, vmem, vmem),
        scratch_shapes=[
            pltpu.VMEM((4, T, dl), bf), pltpu.VMEM((T, D), bf), pltpu.VMEM((T, F), bf),
            pltpu.VMEM((nblk, T, LANES), bf), pltpu.VMEM((nblk, half, LANES), bf),
            pltpu.VMEM((nblk, half, LANES), bf),
            pltpu.VMEM((nb, T, LANES), bf), pltpu.VMEM((nb, T, LANES), bf),
            dma((3, 2, n_fs, len(pieces))), dma((2, n_fs, len(pieces))),
            dma((3,)), dma((4,)),
            dma((nblk,)), dma((nb,)), dma((nblk,)), dma((nblk,)), dma((nblk,)), dma((nb, 2)),
            dma((line + 1,)), dma,
            pltpu.VMEM((r, F), jnp.float32), dma,
        ],
        compiler_params=pltpu.CompilerParams(
            collective_id=0, has_side_effects=True, vmem_limit_bytes=55 * 2 ** 20),
    )(prompt_tokens, norm_gain.reshape(1, r), up_master, down_master)


def solution(mesh):
    n_fs, n_tp = mesh.shape["fs"], mesh.shape["tp"]

    def shards(prompt_tokens, norm_gain, up_master, down_master):
        T, dl = prompt_tokens.shape
        r = up_master.shape[0]
        fits = (n_tp == 4 and n_fs % 2 == 0 and n_fs >= 6 and r % LANES == 0
                and dl % LANES == 0 and T % (2 * LANES) == 0 and r * n_fs == dl * n_tp)
        if not fits:
            return plain(prompt_tokens, norm_gain, up_master, down_master)
        return fused(n_fs, prompt_tokens, norm_gain, up_master, down_master)

    return jax.shard_map(
        shards,
        mesh=mesh,
        in_specs=(P("fs", "tp"), P("fs"), P("fs", "tp"), P("fs", "tp")),
        out_specs=(P(None, "tp"), P(None, "tp"), P("fs", "tp")),
        check_vma=False,
    )
```

```python
import functools

import jax
import jax.numpy as jnp
from jax import lax
from jax.experimental import pallas as pl
from jax.experimental.pallas import tpu as pltpu
from jax.sharding import PartitionSpec as P

MESH = pl.DeviceIdType.MESH
LANES = 128


def plain(prompt_tokens, norm_gain, up_master, down_master):
    up_folded = (norm_gain[:, None] * up_master).astype(jnp.bfloat16)
    down_cast = down_master.astype(jnp.bfloat16)
    whole = lax.all_gather(prompt_tokens, "tp", axis=1, tiled=True)
    width = whole.shape[1]
    hidden_units = up_master.shape[1] * lax.axis_size("tp")
    wide = whole.astype(jnp.float32)
    normed = (wide * lax.rsqrt(jnp.mean(wide * wide, axis=1, keepdims=True) + 1e-05)).astype(
        jnp.bfloat16
    )
    contract = (((1,), (1,)), ((), ()))
    serve_up, serve_down = (
        lax.all_gather(up_folded, "fs", axis=0, tiled=True),
        lax.all_gather(down_cast, "fs", axis=0, tiled=True),
    )
    hidden = jnp.dot(normed, serve_up, preferred_element_type=jnp.float32)
    act = jnp.square(jax.nn.relu(hidden * width ** (-0.5))).astype(jnp.bfloat16)
    product = lax.dot_general(act, serve_down, contract, preferred_element_type=jnp.float32)
    partial_value = (product * hidden_units ** (-0.5)).astype(jnp.bfloat16)
    mixed = lax.psum_scatter(partial_value, "tp", scatter_dimension=1, tiled=True)
    return (serve_up, serve_down, mixed)


def kernel(line, pieces, tok, gain, up, down_hbm, wu, wd, mixed,
           xt, xn, act, part, pbuf, psum, rin_p, rin_y,
           w_send, w_recv, t_send, t_recv, a_send, a_recv, b_send, b_recv, c_send, c_recv,
           o_sem, l_sem, down, d_sem):
    T, dl = tok.shape
    r, F = up.shape
    D = wu.shape[0]
    tp = lax.axis_index("tp")
    fs = lax.axis_index("fs")
    z, x = fs // 2, fs % 2
    core, chip = tp % 2, tp // 2
    partner = tp + 1 - 2 * core
    mirror = (tp + 2) % 4
    diag = (partner + 2) % 4
    has_up, has_dn = z < line - 1, z > 0
    W = (wu, wd)
    nb = dl // LANES
    per = r // LANES
    half = T // 2
    zdev = ((fs + 2, tp), (fs - 2, tp), (fs + 1 - 2 * x, tp))

    own_tok = pltpu.make_async_copy(tok, xt.at[tp], l_sem)
    own_tok.start()
    own_down = pltpu.make_async_copy(down_hbm, down, d_sem)
    own_down.start()

    barrier = pltpu.get_barrier_semaphore()

    def greet(dev):
        pl.semaphore_signal(barrier, inc=1, device_id=dev, device_id_type=MESH)

    for other in (partner, mirror, diag):
        greet((fs, other))
    greet(zdev[2])
    pl.when(has_up)(lambda: greet(zdev[0]))
    pl.when(has_dn)(lambda: greet(zdev[1]))

    base = pl.multiple_of(fs * r, r)
    for i in range(r // LANES):
        rows = slice(i * LANES, (i + 1) * LANES)
        g = jnp.transpose(jnp.broadcast_to(gain[:, rows], (LANES, LANES)))
        for c in range(F // LANES):
            cols = slice(c * LANES, (c + 1) * LANES)
            wu[pl.ds(base + i * LANES, LANES), cols] = (g * up[rows, cols]).astype(jnp.bfloat16)
    links = 4 + has_up.astype(jnp.int32) + has_dn.astype(jnp.int32)
    pl.semaphore_wait(barrier, links)

    def piece(a, s, p, way):
        start, size = pieces[p][0], pieces[p][1]
        ref = W[a].at[pl.ds(pl.multiple_of(s * r + start, 8), size), :]
        return pltpu.make_async_remote_copy(
            src_ref=ref, dst_ref=ref, send_sem=w_send.at[way, a, s, p],
            recv_sem=w_recv.at[a, s, p], device_id=zdev[way], device_id_type=MESH)

    def tok_copy(src, k, slot, to):
        return pltpu.make_async_remote_copy(
            src_ref=src, dst_ref=xt.at[k], send_sem=t_send.at[slot], recv_sem=t_recv.at[k],
            device_id=(fs, to), device_id_type=MESH)

    one = [p for p in range(len(pieces)) if pieces[p][2] == 1]
    two = [p for p in range(len(pieces)) if pieces[p][2] == 2]

    def start(d):
        d.start()

    def wait_send(d):
        d.wait_send()

    def own_z(a, do):
        for p in one + two:
            pl.when(has_up)(lambda: do(piece(a, fs, p, 0)))
            pl.when(has_dn)(lambda: do(piece(a, fs, p, 1)))

    def own_x(a, do):
        for p in two + one:
            do(piece(a, fs, p, 2))

    xs = fs + 1 - 2 * x

    def cross(a, do, wait):
        for p in two:
            if wait:
                piece(a, xs, p, 2).wait_recv()
            pl.when(has_up)(lambda: do(piece(a, xs, p, 0)))
            pl.when(has_dn)(lambda: do(piece(a, xs, p, 1)))

    def place(idx):
        got = jnp.int32(0)
        for i in range(line):
            order = sorted(range(line), key=lambda k: (abs(k - i), -k if i < line / 2 else k))
            for q in range(line):
                got = got + jnp.where((z == i) & (idx == q), jnp.int32(order[q]), jnp.int32(0))
        return got

    def relay(a, idx, do, wait, early=True, late=True):
        zz = place(idx)
        onward_up = (zz < z) & has_up
        onward_dn = (zz > z) & has_dn
        same, cross_s = zz * 2 + x, zz * 2 + 1 - x
        for p in one:
            if not (early if pieces[p][0] < LANES else late):
                continue
            if wait:
                piece(a, same, p, 2).wait_recv()
            pl.when(onward_up)(lambda: do(piece(a, same, p, 0)))
            pl.when(onward_dn)(lambda: do(piece(a, same, p, 1)))
            do(piece(a, same, p, 2))
        for p in two if late else ():
            for s in (same, cross_s):
                if wait:
                    piece(a, s, p, 2).wait_recv()
                pl.when(onward_up)(lambda: do(piece(a, s, p, 0)))
                pl.when(onward_dn)(lambda: do(piece(a, s, p, 1)))

    own_x(0, start)
    own_z(0, start)
    own_tok.wait()
    tok_copy(xt.at[tp], tp, 0, mirror).start()
    tok_copy(xt.at[tp], tp, 1, partner).start()
    own_down.wait()
    wd[pl.ds(base, r), :] = down[...].astype(jnp.bfloat16)
    cross(0, start, True)
    for idx in range(1, line):
        relay(0, jnp.int32(idx), start, True)
        if idx == 1:
            tok_copy(xt.at[mirror], mirror, 0, mirror).wait_recv()
            tok_copy(xt.at[mirror], mirror, 2, partner).start()
    own_z(1, start)
    own_x(1, start)

    tok_copy(xt.at[partner], partner, 1, partner).wait_recv()
    tok_copy(xt.at[diag], diag, 1, partner).wait_recv()
    block = 64

    def norm(i, carry):
        rows = pl.ds(pl.multiple_of(i * block, block), block)
        wide = [xt[k, rows, :].astype(jnp.float32) for k in range(4)]
        sq = wide[0] * wide[0]
        for k in range(1, 4):
            sq = sq + wide[k] * wide[k]
        inv = lax.rsqrt(jnp.sum(sq, axis=1, keepdims=True) * (1.0 / D) + 1e-05)
        for k in range(4):
            xn[rows, k * dl:(k + 1) * dl] = (wide[k] * inv).astype(jnp.bfloat16)
        return carry

    lax.fori_loop(0, T // block, norm, 0)

    cross(1, start, True)
    for idx in range(line):
        s = place(jnp.int32(idx)) * 2 + 1 - x
        for p in one:
            piece(0, s, p, 2).wait_recv()

    mrows = 2 * LANES

    def first(i, carry):
        rows = pl.ds(pl.multiple_of(i * mrows, mrows), mrows)
        hidden = jnp.dot(xn[rows, :], wu[...], preferred_element_type=jnp.float32) * D ** (-0.5)
        hidden = jnp.maximum(hidden, 0.0)
        act[rows, :] = (hidden * hidden).astype(jnp.bfloat16)
        return carry

    lax.fori_loop(0, T // mrows, first, 0)

    scale = (F * 4) ** (-0.5)
    mine = pl.ds(pl.multiple_of(core * half, half), half)
    theirs = pl.ds(pl.multiple_of((1 - core) * half, half), half)
    steps = 2 * per
    inner = has_up & has_dn

    def turn(n):
        idx, j = n // steps, n % steps
        last = idx == line - 1
        return jnp.where(last, j % 2, j // per), jnp.where(last, j // 2, j % per)

    def block_of(n):
        side, h = turn(n)
        s = place(n // steps) * 2 + x + side * (1 - 2 * x)
        return s * per + h

    def owner_of(b):
        o = b // nb
        return o, (o // 2) == chip

    def to_partner(b):
        return pltpu.make_async_remote_copy(
            src_ref=part.at[b], dst_ref=rin_p.at[b % nb], send_sem=a_send.at[b],
            recv_sem=a_recv.at[b % nb], device_id=(fs, partner), device_id_type=MESH)

    def swap(b):
        return pltpu.make_async_remote_copy(
            src_ref=part.at[b, theirs, :], dst_ref=pbuf.at[b], send_sem=b_send.at[b],
            recv_sem=b_recv.at[b], device_id=(fs, partner), device_id_type=MESH)

    def to_owner(b, o):
        return pltpu.make_async_remote_copy(
            src_ref=psum.at[b], dst_ref=rin_y.at[b % nb, mine, :], send_sem=c_send.at[b],
            recv_sem=c_recv.at[b % nb, core], device_id=(fs, o), device_id_type=MESH)

    def second_half(b):
        o, here = owner_of(b)

        @pl.when(jnp.logical_not(here))
        def _():
            swap(b).wait_recv()
            psum[b] = (part[b, mine, :].astype(jnp.float32)
                       + pbuf[b].astype(jnp.float32)).astype(jnp.bfloat16)
            to_owner(b, o).start()

    def body(n, carry):
        idx, j = n // steps, n % steps

        @pl.when((j == per) & (idx + 1 < line))
        def _():
            relay(1, idx + 1, start, True, late=False)

        @pl.when((j == per) & (idx + 1 < line) & (inner | (idx + 2 < line)))
        def _():
            relay(1, idx + 1, start, True, early=False)

        @pl.when((j == steps - 2) & (idx == line - 1) & jnp.logical_not(inner))
        def _():
            relay(1, idx, start, True, early=False)

        side, at = turn(n)
        far = place(idx) * 2 + 1 - x
        for h in range(per):
            @pl.when((side == 1) & (at == h))
            def _():
                for p in one:
                    if pieces[p][0] // LANES == h:
                        piece(1, far, p, 2).wait_recv()
        b = block_of(n)
        rhs = wd[pl.ds(pl.multiple_of(b * LANES, LANES), LANES), :]
        product = lax.dot_general(act[...], rhs, (((1,), (1,)), ((), ())),
                                  preferred_element_type=jnp.float32)
        part[b] = (product * scale).astype(jnp.bfloat16)
        o, here = owner_of(b)

        @pl.when(here & (o != tp))
        def _():
            to_partner(b).start()

        @pl.when(jnp.logical_not(here))
        def _():
            swap(b).start()

        @pl.when(n > 0)
        def _():
            second_half(block_of(n - 1))

        return carry

    total = line * steps
    lax.fori_loop(0, total, body, 0)
    second_half(block_of(jnp.int32(total - 1)))

    for i in range(nb):
        b = tp * nb + i
        to_partner(b).wait_recv()
        for c in range(2):
            pltpu.make_async_remote_copy(
                src_ref=psum.at[b], dst_ref=rin_y.at[i, c * half:(c + 1) * half, :],
                send_sem=c_send.at[b], recv_sem=c_recv.at[i, c],
                device_id=(fs, partner), device_id_type=MESH).wait_recv()
        mixed[:, i * LANES:(i + 1) * LANES] = (
            part[b].astype(jnp.float32) + rin_p[i].astype(jnp.float32)
            + rin_y[i].astype(jnp.float32)).astype(jnp.bfloat16)

    for slot, (k, to) in enumerate(((tp, mirror), (tp, partner), (mirror, partner))):
        tok_copy(xt.at[k], k, slot, to).wait_send()
    for a in range(2):
        own_x(a, wait_send)
        own_z(a, wait_send)
        cross(a, wait_send, False)

    def drain(idx, carry):
        for a in range(2):
            relay(a, idx, wait_send, False)
        return carry

    lax.fori_loop(1, line, drain, 0)

    def drain_sums(b, carry):
        o, here = owner_of(b)

        @pl.when(here & (o != tp))
        def _():
            to_partner(b).wait_send()

        @pl.when(jnp.logical_not(here))
        def _():
            swap(b).wait_send()
            to_owner(b, o).wait_send()

        return carry

    lax.fori_loop(0, D // LANES, drain_sums, 0)


def cut(r):
    across = min(LANES - 16, max(16, r * 5 // 32 // 8 * 8))
    got = []
    for first in range(0, r, LANES):
        rows = LANES if first + LANES < r else LANES - across
        if rows == LANES:
            got += [(first, LANES // 2, 1), (first + LANES // 2, LANES // 2, 1)]
        else:
            got += [(first, rows, 1)]
    return got + [(r - across, across, 2)]


def fused(n_fs, prompt_tokens, norm_gain, up_master, down_master):
    T, dl = prompt_tokens.shape
    r, F = up_master.shape
    D = r * n_fs
    line = n_fs // 2
    pieces = cut(r)
    nblk, nb, half = D // LANES, dl // LANES, T // 2
    bf = jnp.bfloat16
    dma = pltpu.SemaphoreType.DMA
    vmem = pl.BlockSpec(memory_space=pltpu.VMEM)
    hbm = pl.BlockSpec(memory_space=pl.ANY)
    return pl.pallas_call(
        functools.partial(kernel, line, pieces),
        out_shape=(pltpu.VMEM((D, F), bf), pltpu.VMEM((D, F), bf), pltpu.VMEM((T, dl), bf)),
        in_specs=[hbm, vmem, vmem, hbm],
        out_specs=(vmem, vmem, vmem),
        scratch_shapes=[
            pltpu.VMEM((4, T, dl), bf), pltpu.VMEM((T, D), bf), pltpu.VMEM((T, F), bf),
            pltpu.VMEM((nblk, T, LANES), bf), pltpu.VMEM((nblk, half, LANES), bf),
            pltpu.VMEM((nblk, half, LANES), bf),
            pltpu.VMEM((nb, T, LANES), bf), pltpu.VMEM((nb, T, LANES), bf),
            dma((3, 2, n_fs, len(pieces))), dma((2, n_fs, len(pieces))),
            dma((3,)), dma((4,)),
            dma((nblk,)), dma((nb,)), dma((nblk,)), dma((nblk,)), dma((nblk,)), dma((nb, 2)),
            dma((line + 1,)), dma,
            pltpu.VMEM((r, F), jnp.float32), dma,
        ],
        compiler_params=pltpu.CompilerParams(
            collective_id=0, has_side_effects=True, vmem_limit_bytes=55 * 2 ** 20),
    )(prompt_tokens, norm_gain.reshape(1, r), up_master, down_master)


def put(src_a, src_b, src_c, dst_a, dst_b, dst_c, sem):
    copies = []
    for src, dst in ((src_a, dst_a), (src_b, dst_b), (src_c, dst_c)):
        n = 4 if src is not src_c else 1
        rows = src.shape[0] // n
        for i in range(n):
            part = pl.ds(i * rows, rows)
            copies.append(pltpu.make_async_copy(
                src.at[part, :], dst.at[part, :], sem.at[len(copies)]))
    for c in copies:
        c.start()
    for c in copies:
        c.wait()


def written(*arrays):
    hbm = pl.BlockSpec(memory_space=pl.ANY)
    return pl.pallas_call(
        put,
        out_shape=tuple(pltpu.HBM(a.shape, a.dtype) for a in arrays),
        in_specs=[pl.BlockSpec(memory_space=pltpu.VMEM)] * 3,
        out_specs=(pl.BlockSpec(memory_space=pltpu.HBM),) * 3,
        scratch_shapes=[pltpu.SemaphoreType.DMA((9,))],
        compiler_params=pltpu.CompilerParams(vmem_limit_bytes=2 ** 20),
    )(*(pltpu.with_memory_space_constraint(a, pltpu.VMEM) for a in arrays))


def solution(mesh):
    n_fs, n_tp = mesh.shape["fs"], mesh.shape["tp"]

    def shards(prompt_tokens, norm_gain, up_master, down_master):
        T, dl = prompt_tokens.shape
        r = up_master.shape[0]
        fits = (n_tp == 4 and n_fs % 2 == 0 and n_fs >= 6 and r % LANES == 0
                and dl % LANES == 0 and T % (2 * LANES) == 0 and r * n_fs == dl * n_tp)
        if not fits:
            return plain(prompt_tokens, norm_gain, up_master, down_master)
        return written(*fused(n_fs, prompt_tokens, norm_gain, up_master, down_master))

    return jax.shard_map(
        shards,
        mesh=mesh,
        in_specs=(P("fs", "tp"), P("fs"), P("fs", "tp"), P("fs", "tp")),
        out_specs=(P(None, "tp"), P(None, "tp"), P("fs", "tp")),
        check_vma=False,
    )
```
